32 devices in a mesh: sp: 8 (over z, x), tp: 4 (over y, core).
Axes of the slice: x: 2, y: 2, z: 4, core: 2. Of those that a mesh axis runs over, the one named last changes fastest.
Arguments:
- tokens: bfloat16 [3072, 2048], P('sp', 'tp'), may hold values from -6 to 6
- pre_gain: float32 [2048], replicated, may hold values from 0.1 to 1.9
- outer_gate_weight: bfloat16 [2048, 1024], P(None, 'tp'), may hold values from -0.125 to 0.125
- inner_gate_weight: bfloat16 [2048, 1024], P(None, 'tp'), may hold values from -0.125 to 0.125
- source_weight: bfloat16 [2048, 1024], P(None, 'tp'), may hold values from -0.125 to 0.125
- conv_taps: bfloat16 [3, 1024], P(None, 'tp'), may hold values from -3.5 to 3.5
- q_down_weight: bfloat16 [2048, 768], replicated, may hold values from -0.125 to 0.125
- q_norm_gain: float32 [768], replicated, may hold values from 0.5 to 16
- q_up_weight: bfloat16 [768, 3072], P(None, 'tp'), may hold values from -0.21875 to 0.21875
- kv_down_weight: bfloat16 [2048, 512], replicated, may hold values from -0.125 to 0.125
- rope_key_weight: bfloat16 [2048, 32], replicated, may hold values from -0.125 to 0.125
- kv_norm_gain: float32 [512], replicated, may hold values from 0.5 to 16
- kv_up_weight: bfloat16 [512, 4096], P(None, 'tp'), may hold values from -0.25 to 0.25
- attn_out_weight: bfloat16 [2048, 2048], P('tp'), may hold values from -4 to 4
- conv_out_weight: bfloat16 [1024, 2048], P('tp'), may hold values from -0.1875 to 0.1875
- post_gain: float32 [2048], P('tp'), may hold values from 0.1 to 1.9
Outputs:
- mixed: bfloat16 [3072, 2048], P('sp', 'tp')
- log_total: float32 [32, 3072], P('tp', 'sp')
The draws below stay inside these ranges and needn't reach their ends.
All inputs are finite; a program needn't handle non-finite values.
Results may differ from the reference program's by a relative error of at most 0.017.
The reference program's roundings to bfloat16 on the way count: a program that leaves them out, or rounds other values in their place, can miss the bound.
Values may be sent and summed in bfloat16 or wider, within the bound.
A program may use at most 128 MiB of HBM per device.

```python
import jax
import jax.numpy as jnp
from jax import lax

D = 2048
HEADS = 32
NOPE = 64
ROPE = 32
VDIM = 64
Q_RANK = 768
KV_RANK = 512
CONV_W = 1024
TAPS = 3
TOK_DEV = 384
TOKENS = 3072
N_SP = 8
N_TP = 4


def latent_gain(key, count):
    upper = 2.0
    return jnp.exp(jax.random.uniform(key, (count,), jnp.float32, jnp.log(0.5), jnp.log(upper)))


def draw_q_norm_gain(key, part):
    return latent_gain(jax.random.fold_in(key, 11), Q_RANK)


def draw_kv_norm_gain(key, part):
    return latent_gain(jax.random.fold_in(key, 23), KV_RANK)


def block_levels(stream_key, shape, shards, low, high):
    gain, own = 1.0, jax.random.fold_in(stream_key, 6)
    for dim, parts in shards:
        steps = jnp.exp(jax.random.uniform(jax.random.fold_in(own, dim), (parts,), jnp.float32, low / len(shards), high / len(shards)))
        gain = gain * jnp.repeat(steps, shape[dim] // parts).reshape([-1 if axis == dim else 1 for axis in range(len(shape))])
    return gain


def centred(stream_key, dims, scale, bound, split=(), held_as=jnp.bfloat16):
    values = scale * jax.random.normal(stream_key, dims, jnp.float32)
    if split:
        values = values * block_levels(stream_key, dims, split, -0.22, 0.18)
    return jnp.clip(values, -bound, bound).astype(held_as)


def setup_inputs(seed: int = 0) -> dict:
    splits = jax.random.split(jax.random.key(seed), 17)
    return {
        "tokens": centred(splits[0], (TOKENS, D), 1.0, 6.0, ((0, 8), (1, 4))),
        "pre_gain": jnp.clip(1.0 + 0.18 * jax.random.normal(splits[1], (D,), jnp.float32), 0.1, 1.9),
        "outer_gate_weight": centred(splits[2], (D, CONV_W), D ** -0.5, 0.125, ((1, 4),)),
        "inner_gate_weight": centred(splits[3], (D, CONV_W), D ** -0.5, 0.125, ((1, 4),)),
        "source_weight": centred(splits[4], (D, CONV_W), D ** -0.5, 0.125, ((1, 4),)),
        "conv_taps": centred(splits[5], (TAPS, CONV_W), TAPS ** -0.5, 3.5, ((1, 4),)),
        "q_down_weight": centred(splits[6], (D, Q_RANK), D ** -0.5, 0.125),
        "q_norm_gain": draw_q_norm_gain(jax.random.fold_in(splits[16], 71), 0),
        "q_up_weight": centred(splits[8], (Q_RANK, HEADS * (NOPE + ROPE)), Q_RANK ** -0.5, 0.21875, ((1, 4),)),
        "kv_down_weight": centred(splits[9], (D, KV_RANK), D ** -0.5, 0.125),
        "rope_key_weight": centred(splits[10], (D, ROPE), D ** -0.5, 0.125),
        "kv_norm_gain": draw_kv_norm_gain(jax.random.fold_in(splits[16], 71), 0),
        "kv_up_weight": centred(splits[12], (KV_RANK, HEADS * (NOPE + VDIM)), KV_RANK ** -0.5, 0.25, ((1, 4),)),
        "attn_out_weight": centred(splits[13], (HEADS * VDIM, D), 2 ** -0.5, 4.0, ((0, 4),)),
        "conv_out_weight": centred(splits[14], (CONV_W, D), CONV_W ** -0.5, 0.1875, ((0, 4),)),
        "post_gain": jnp.clip(1.0 + 0.18 * jax.random.normal(splits[15], (D,), jnp.float32), 0.1, 1.9),
    }


EPSILON = 1e-06
THETA = 500000.0

def rms_scale(values):
    return lax.rsqrt(lax.optimization_barrier(jnp.mean(values * values, axis=-1, keepdims=True)) + EPSILON)

def rotation(positions, width):
    freqs = THETA ** (-jnp.arange(0, width, 2, dtype=jnp.float32) / width)
    angles = positions.astype(jnp.float32)[:, None] * freqs[None, :]
    return (jnp.cos(angles), jnp.sin(angles))

def rotate(values, cosine, sine):
    half = values.shape[-1] // 2
    first = values[..., :half]
    second = values[..., half:]
    return jnp.concatenate([first * cosine - second * sine, second * cosine + first * sine], axis=-1)

def reference(tokens, pre_gain, outer_gate_weight, inner_gate_weight, source_weight, conv_taps, q_down_weight, q_norm_gain, q_up_weight, kv_down_weight, rope_key_weight, kv_norm_gain, kv_up_weight, attn_out_weight, conv_out_weight, post_gain):
    wide = tokens.astype(jnp.float32)
    scaled = (wide * pre_gain).astype(jnp.bfloat16)
    factor = rms_scale(wide)

    def project(weight):
        return jnp.dot(scaled, weight, preferred_element_type=jnp.float32) * factor
    outer = project(outer_gate_weight).astype(jnp.bfloat16)
    inner = project(inner_gate_weight).astype(jnp.bfloat16)
    source = project(source_weight).astype(jnp.bfloat16)
    driven = (inner.astype(jnp.float32) * source.astype(jnp.float32)).astype(jnp.bfloat16)
    padded = jnp.concatenate([jnp.zeros((TAPS - 1, CONV_W), jnp.bfloat16), driven], axis=0)
    convolved = jnp.zeros((TOKENS, CONV_W), jnp.float32)
    for index in range(TAPS):
        convolved = convolved + conv_taps[index].astype(jnp.float32) * padded[index:index + TOKENS].astype(jnp.float32)
    conv_branch = (outer.astype(jnp.float32) * convolved).astype(jnp.bfloat16)
    positions = jnp.arange(TOKENS, dtype=jnp.int32)
    cosine, sine = rotation(positions, ROPE)
    q_latent = project(q_down_weight)
    q_normed = (q_latent * rms_scale(q_latent) * q_norm_gain).astype(jnp.bfloat16)
    query = jnp.dot(q_normed, q_up_weight, preferred_element_type=jnp.float32).reshape(TOKENS, HEADS, NOPE + ROPE)
    q_plain = query[..., :NOPE].astype(jnp.bfloat16)
    q_turned = rotate(query[..., NOPE:], cosine[:, None], sine[:, None]).astype(jnp.bfloat16)
    kv_latent = project(kv_down_weight)
    latent = (kv_latent * rms_scale(kv_latent) * kv_norm_gain).astype(jnp.bfloat16)
    rope_key = rotate(project(rope_key_weight), cosine, sine).astype(jnp.bfloat16)
    keyvals = jnp.dot(latent, kv_up_weight, preferred_element_type=jnp.float32).astype(jnp.bfloat16)
    keyvals = keyvals.reshape(TOKENS, HEADS, NOPE + VDIM)
    head_plain = jnp.transpose(q_plain, (1, 0, 2))
    head_turned = jnp.transpose(q_turned, (1, 0, 2))
    head_keys = jnp.transpose(keyvals[..., :NOPE], (1, 0, 2))
    head_values = jnp.transpose(keyvals[..., NOPE:], (1, 0, 2))
    scale = (NOPE + ROPE) ** (-0.5)
    outputs = []
    logs = []
    for block in range(N_SP):
        first = block * TOK_DEV
        last = first + TOK_DEV
        key_turned = rope_key[:last]
        query_pos = jnp.arange(first, last, dtype=jnp.int32)
        key_pos = jnp.arange(last, dtype=jnp.int32)
        allowed = key_pos[None, :] <= query_pos[:, None]

        def per_head(items):
            plain, turned, keys, values = items
            scores = jnp.dot(plain, keys.T, preferred_element_type=jnp.float32)
            scores = scores + jnp.dot(turned, key_turned.T, preferred_element_type=jnp.float32)
            scores = jnp.where(allowed, scores * scale, -jnp.inf)
            maxima = lax.optimization_barrier(jnp.max(scores, axis=-1, keepdims=True))
            weights = jnp.exp(scores - maxima)
            totals = lax.optimization_barrier(jnp.sum(weights, axis=-1))
            result = jnp.dot(weights.astype(jnp.bfloat16), values, preferred_element_type=jnp.float32) / totals[:, None]
            return (result.astype(jnp.bfloat16), maxima[:, 0] + jnp.log(totals))
        block_out, block_log = lax.map(per_head, (head_plain[:, first:last], head_turned[:, first:last], head_keys[:, :last], head_values[:, :last]))
        outputs.append(block_out)
        logs.append(block_log)
    attended = jnp.concatenate(outputs, axis=1)
    log_total = jnp.concatenate(logs, axis=1)
    attended = jnp.transpose(attended, (1, 0, 2)).reshape(TOKENS, HEADS * VDIM)
    head_rows = HEADS // N_TP * VDIM
    channel_rows = CONV_W // N_TP
    projected = jnp.zeros((TOKENS, D), jnp.float32)
    for group in range(N_TP):
        head_part = jnp.dot(attended[:, group * head_rows:(group + 1) * head_rows], attn_out_weight[group * head_rows:(group + 1) * head_rows], preferred_element_type=jnp.float32)
        conv_part = jnp.dot(conv_branch[:, group * channel_rows:(group + 1) * channel_rows], conv_out_weight[group * channel_rows:(group + 1) * channel_rows], preferred_element_type=jnp.float32)
        rounded = lax.optimization_barrier((head_part + conv_part).astype(jnp.bfloat16))
        projected = projected + rounded.astype(jnp.float32)
    mixed = (projected * rms_scale(projected) * post_gain).astype(jnp.bfloat16)
    return (mixed, log_total)
```

```python
import functools
import math

import jax
import jax.numpy as jnp
from jax import lax
from jax.experimental import pallas as pl
from jax.experimental.pallas import tpu as pltpu
from jax.sharding import PartitionSpec as P

NOPE = 64
ROPE = 32
VDIM = 64
TAPS = 3
LANES = 128

EPSILON = 1e-06
THETA = 500000.0
NEGATIVE = -1e30
MESH = pl.DeviceIdType.MESH
BF = jnp.bfloat16
F32 = jnp.float32


def remote(src, dst, send, recv, **where):
    return pltpu.make_async_remote_copy(
        src_ref=src, dst_ref=dst, send_sem=send, recv_sem=recv, device_id=where, device_id_type=MESH
    )


def dot(a, b):
    return jnp.dot(a, b, preferred_element_type=F32)


def greet_tp(tp, n):
    barrier = pltpu.get_barrier_semaphore()
    for step in range(1, n):
        pl.semaphore_signal(
            barrier, inc=1, device_id={"tp": lax.rem(tp + step, n)}, device_id_type=MESH
        )
    pl.semaphore_wait(barrier, n - 1)


def project_kernel(
    n, chunk,
    tok, pre, qg, kg, cos, sin, wo, wi, ws, wq, wk, wr,
    outer, driven, qn, kvb,
    buf, vo, vi, vs, vq, vk, vr, wsem, own_s, own_r, y_s, y_r, f_s, f_r,
):
    tp = lax.axis_index("tp")
    ny = n // 2
    y, core = tp // 2, lax.rem(tp, 2)
    partner = tp + 1 - 2 * core
    rows, width = tok.shape
    count = rows // chunk
    loads = [
        pltpu.make_async_copy(a, b, wsem.at[i])
        for i, (a, b) in enumerate(((wo, vo), (wi, vi), (ws, vs), (wq, vq), (wk, vk), (wr, vr)))
    ]
    greet_tp(tp, n)

    def part(r):
        return pl.ds(r * chunk, chunk)

    def y_copy(r, step):
        to = lax.rem(y + step, ny) * 2 + core
        return remote(
            tok.at[part(r)], buf.at[tp, part(r)], y_s.at[r, step], y_r.at[r, y], tp=to
        )

    def y_arrival(r, other):
        return remote(
            tok.at[part(r)], buf.at[other * 2 + core, part(r)], y_s.at[r, 0], y_r.at[r, other],
            tp=partner,
        )

    def own_copy(r):
        return remote(tok.at[part(r)], buf.at[tp, part(r)], own_s.at[r], own_r.at[r], tp=partner)

    def forward(r, other):
        here = buf.at[other * 2 + core, part(r)]
        return remote(here, here, f_s.at[r, other], f_r.at[r, other], tp=partner)

    for r in range(count):
        for step in range(1, ny):
            y_copy(r, step).start()
    for r in range(count):
        own_copy(r).start()
    for load in loads:
        load.start()
    buf[tp] = tok[...]
    for load in loads:
        load.wait()

    def compute(r, carry):
        for step in range(1, ny):
            other = lax.rem(y + ny - step, ny)
            y_arrival(r, other).wait_recv()
            forward(r, other).start()
        own_copy(r).wait_recv()
        for step in range(1, ny):
            other = lax.rem(y + ny - step, ny)
            forward(r, other).wait_recv()
        here = pl.ds(pl.multiple_of(r * chunk, chunk), chunk)
        total = n * width
        wide = jnp.concatenate([buf[s, here] for s in range(n)], axis=1).astype(F32)
        factor = lax.rsqrt(jnp.sum(wide * wide, axis=1, keepdims=True) / total + EPSILON)
        scaled = (wide * pre[...]).astype(BF)
        kv = dot(scaled, vk[...]) * factor
        kv = kv * lax.rsqrt(jnp.mean(kv * kv, axis=1, keepdims=True) + EPSILON) * kg[...]
        rank = kv.shape[1]
        kvb[here, :rank] = kv.astype(BF)
        turn = dot(scaled, vr[...]) * factor
        swapped = jnp.concatenate([turn[:, ROPE // 2 :], turn[:, : ROPE // 2]], axis=1)
        turn = turn * cos[here] + swapped * sin[here]
        kvb[here, rank:] = jnp.concatenate(
            [turn, jnp.zeros((chunk, LANES - ROPE), F32)], axis=1
        ).astype(BF)
        q = dot(scaled, vq[...]) * factor
        q = q * lax.rsqrt(jnp.mean(q * q, axis=1, keepdims=True) + EPSILON) * qg[...]
        qn[here] = q.astype(BF)
        outer[here] = (dot(scaled, vo[...]) * factor).astype(BF)
        inner = (dot(scaled, vi[...]) * factor).astype(BF).astype(F32)
        source = (dot(scaled, vs[...]) * factor).astype(BF).astype(F32)
        driven[here] = (inner * source).astype(BF)
        return carry

    lax.fori_loop(0, count, compute, 0)
    for r in range(count):
        own_copy(r).wait_send()
        for step in range(1, ny):
            y_copy(r, step).wait_send()
            forward(r, lax.rem(y + step, ny)).wait_send()


def attend_kernel(
    nz, nx, ntp, heads,
    kvb, qt, up,
    att, logs,
    buf, kv, acc, top, low, z_s, x_s, d_s, i_r, d_r,
):
    sp, tp = lax.axis_index("sp"), lax.axis_index("tp")
    z, x = sp // nx, lax.rem(sp, nx)
    core = lax.rem(tp, 2)
    partner = tp + 1 - 2 * core
    rows = kvb.shape[0]
    half = rows // 2
    rank = up.shape[0]
    scale = (NOPE + ROPE) ** (-0.5)
    factor = scale * math.log2(math.e)
    mine = pl.ds(pl.multiple_of(core * half, half), half)

    barrier = pltpu.get_barrier_semaphore()

    def greet(**where):
        pl.semaphore_signal(barrier, inc=1, device_id=where, device_id_type=MESH)

    greet(tp=partner)
    for step in range(1, nx):
        greet(sp=z * nx + lax.rem(x + step, nx))

    @pl.when(z > 0)
    def _():
        greet(sp=sp - nx)

    @pl.when(z < nz - 1)
    def _():
        greet(sp=sp + nx)

    inside = jnp.where(z > 0, 1, 0) + jnp.where(z < nz - 1, 1, 0)
    pl.semaphore_wait(barrier, nx + inside)

    def up_copy(k):
        src = sp - k * nx
        return remote(buf.at[src, mine], buf.at[src, mine], z_s.at[k], i_r.at[src], sp=sp + nx)

    def side_copy(k, step):
        src = sp - k * nx
        to = z * nx + lax.rem(x + step, nx)
        return remote(buf.at[src, mine], buf.at[src, mine], x_s.at[k, step], i_r.at[src], sp=to)

    def own_up():
        return remote(kvb.at[mine], buf.at[sp, mine], z_s.at[0], i_r.at[sp], sp=sp + nx)

    def own_side(step):
        to = z * nx + lax.rem(x + step, nx)
        return remote(kvb.at[mine], buf.at[sp, mine], x_s.at[0, step], i_r.at[sp], sp=to)

    def arrival(src):
        return remote(kvb.at[mine], buf.at[src, mine], z_s.at[0], i_r.at[src], tp=partner)

    def share(src):
        return remote(buf.at[src, mine], buf.at[src, mine], d_s.at[src], d_r.at[src], tp=partner)

    @pl.when(z < nz - 1)
    def _():
        own_up().start()

    for step in range(1, nx):
        @pl.when(x + step < nx)
        def _(step=step):
            own_side(step).start()

    def compute(block, first):
        lat = block[:, :rank]
        turn = block[:, rank:]
        for h in range(heads):
            kv[h] = dot(lat, up[:, h * LANES : (h + 1) * LANES]).astype(BF)

        def one(h):
            keyval = kv[h]
            scores = dot(jnp.concatenate([keyval, turn], axis=1), qt[h])
            if first:
                key = lax.broadcasted_iota(jnp.int32, scores.shape, 0)
                query = lax.broadcasted_iota(jnp.int32, scores.shape, 1)
                scores = jnp.where(key <= query, scores, NEGATIVE)
            peak = jnp.max(scores, axis=0, keepdims=True) * factor
            if not first:
                before = top[h]
                peak = jnp.maximum(before, peak)
            weights = jnp.exp2(scores * factor - peak)
            total = jnp.sum(weights, axis=0, keepdims=True)
            values = lax.dot_general(
                keyval, weights.astype(BF), (((0,), (0,)), ((), ())), preferred_element_type=F32
            )
            if not first:
                shrink = jnp.exp2(before - peak)
                total = total + low[h] * shrink
                values = values + acc[h] * shrink
            top[h] = peak
            low[h] = total
            acc[h] = values

        def pair(i, carry):
            one(2 * i)
            one(2 * i + 1)
            return carry

        lax.fori_loop(0, heads // 2, pair, 0)

    compute(kvb[...], True)

    def receive_side(src):
        arrival(src).wait_recv()
        share(src).start()
        share(src).wait_recv()
        compute(buf[src], False)

    def side_loop(k, low_step):
        def run(step, carry):
            receive_side((z - k) * nx + lax.rem(x + step, nx))
            return carry

        lax.fori_loop(low_step, nx, run, 0)

    side_loop(0, nx - x)

    def level(k, carry):
        src = sp - k * nx
        arrival(src).wait_recv()

        @pl.when(z < nz - 1)
        def _():
            up_copy(k).start()

        for step in range(1, nx):
            side_copy(k, step).start()
        share(src).start()
        share(src).wait_recv()
        compute(buf[src], False)
        side_loop(k, 1)
        return carry

    lax.fori_loop(1, z + 1, level, 0)

    for i in range(heads // 2):
        both = jnp.concatenate(
            [acc[2 * i, NOPE:] / low[2 * i], acc[2 * i + 1, NOPE:] / low[2 * i + 1]], axis=0
        )
        att[:, i * LANES : (i + 1) * LANES] = both.T.astype(BF)
    for h in range(heads):
        logs[h : h + 1, :] = top[h] * math.log(2.0) + jnp.log(low[h])

    @pl.when(z < nz - 1)
    def _():
        own_up().wait_send()

    for step in range(1, nx):
        @pl.when(x + step < nx)
        def _(step=step):
            own_side(step).wait_send()

    def side_sent(k, low_step):
        def run(step, carry):
            share((z - k) * nx + lax.rem(x + step, nx)).wait_send()
            return carry

        lax.fori_loop(low_step, nx, run, 0)

    side_sent(0, nx - x)

    def sent(k, carry):
        @pl.when(z < nz - 1)
        def _():
            up_copy(k).wait_send()

        for step in range(1, nx):
            side_copy(k, step).wait_send()
        share(sp - k * nx).wait_send()
        side_sent(k, 1)
        return carry

    lax.fori_loop(1, z + 1, sent, 0)


def finish_kernel(
    n, chunk,
    att, conv, wa, wc, gain,
    out,
    away, mine, pin, ysend, yin, peer, pown, total, sq, sqin,
    a_s, a_r, y_s, y_r, p_s, p_r, q_s, q_r,
):
    tp = lax.axis_index("tp")
    ny = n // 2
    y, core = tp // 2, lax.rem(tp, 2)
    partner = tp + 1 - 2 * core
    rows, width = out.shape
    count = rows // chunk
    greet_tp(tp, n)

    def part(r):
        return pl.ds(r * chunk, chunk)

    def product(r, dest):
        columns = pl.ds(pl.multiple_of(dest * width, width), width)
        return (dot(att[part(r)], wa[:, columns]) + dot(conv[part(r)], wc[:, columns])).astype(BF)

    def to_partner(r, step):
        return remote(
            away.at[step, part(r)], pin.at[step, part(r)], a_s.at[r, step], a_r.at[r, step], tp=partner
        )

    def across(r, step):
        to = lax.rem(y + step, ny) * 2 + core
        return remote(
            ysend.at[step, part(r)], yin.at[step, part(r)], y_s.at[r, step], y_r.at[r, step], tp=to
        )

    def home(r):
        return remote(peer.at[part(r)], pown.at[part(r)], p_s.at[r], p_r.at[r], tp=partner)

    def squares(step):
        return remote(
            sq, sqin.at[step], q_s.at[step], q_r.at[step], tp=lax.rem(tp + step, n)
        )

    for r in range(count):
        for step in range(1, ny):
            dest = lax.rem(y + step, ny) * 2
            away[step, part(r)] = product(r, dest + 1 - core)
            to_partner(r, step).start()
            mine[step, part(r)] = product(r, dest + core)
    for r in range(count):
        for step in range(1, ny):
            to_partner(r, step).wait_recv()
            ysend[step, part(r)] = (
                mine[step, part(r)].astype(F32) + pin[step, part(r)].astype(F32)
            ).astype(BF)
            across(r, step).start()
    for r in range(count):
        peer[part(r)] = product(r, partner)
        home(r).start()
        total[part(r)] = product(r, tp).astype(F32)
    for r in range(count):
        home(r).wait_recv()
        total[part(r)] += pown[part(r)].astype(F32)
    for r in range(count):
        for step in range(1, ny):
            across(r, step).wait_recv()
            total[part(r)] += yin[step, part(r)].astype(F32)
        value = total[part(r)]
        sums = jnp.sum(value * value, axis=1, keepdims=True)
        sq[:, part(r)] = jnp.broadcast_to(sums, (chunk, LANES)).T[:8]
    for step in range(1, n):
        squares(step).start()
    whole = sq[...]
    for step in range(1, n):
        squares(step).wait_recv()
        whole = whole + sqin[step]
    scale = lax.rsqrt(whole / (n * width) + EPSILON)
    for r in range(count):
        column = jnp.broadcast_to(
            scale[:1, r * chunk : (r + 1) * chunk], (LANES, chunk)
        ).T[:, :1]
        out[part(r)] = (total[part(r)] * column * gain[...]).astype(BF)
    for r in range(count):
        home(r).wait_send()
        for step in range(1, ny):
            to_partner(r, step).wait_send()
            across(r, step).wait_send()
    for step in range(1, n):
        squares(step).wait_send()


def vmem(count):
    return [pl.BlockSpec(memory_space=pltpu.VMEM)] * count


def params(collective):
    return pltpu.CompilerParams(
        collective_id=collective, has_side_effects=True, vmem_limit_bytes=56 * 1024 * 1024
    )


DMA = pltpu.SemaphoreType.DMA


def body(
    nsp, ntp,
    tokens, pre_gain, outer_gate_weight, inner_gate_weight, source_weight, conv_taps,
    q_down_weight, q_norm_gain, q_up_weight, kv_down_weight, rope_key_weight, kv_norm_gain,
    kv_up_weight, attn_out_weight, conv_out_weight, post_gain,
):
    rows, width = tokens.shape
    ny = ntp // 2
    nx = ny if nsp % ny == 0 else 1
    nz = nsp // nx
    chunk = LANES
    count = rows // chunk
    q_rank, kv_rank = q_down_weight.shape[1], kv_down_weight.shape[1]
    channels = outer_gate_weight.shape[1]
    heads = q_up_weight.shape[1] // (NOPE + ROPE)
    struct = jax.ShapeDtypeStruct
    sp = lax.axis_index("sp")

    pos = (sp * rows + jnp.arange(rows, dtype=jnp.int32)).astype(F32)
    freqs = THETA ** (-jnp.arange(0, ROPE, 2, dtype=F32) / ROPE)
    angles = pos[:, None] * freqs[None, :]
    cosine, sine = jnp.cos(angles), jnp.sin(angles)
    cos_full = jnp.concatenate([cosine, cosine], axis=1)
    sin_full = jnp.concatenate([-sine, sine], axis=1)

    weights = (
        outer_gate_weight, inner_gate_weight, source_weight,
        q_down_weight, kv_down_weight, rope_key_weight,
    )
    outer, driven, q_normed, kvb = pl.pallas_call(
        functools.partial(project_kernel, ntp, chunk),
        out_shape=[
            struct((rows, channels), BF), struct((rows, channels), BF),
            struct((rows, q_rank), BF), struct((rows, kv_rank + LANES), BF),
        ],
        in_specs=vmem(6) + [pl.BlockSpec(memory_space=pl.ANY)] * 6,
        out_specs=vmem(4),
        scratch_shapes=[pltpu.VMEM((ntp, rows, width), BF)]
        + [pltpu.VMEM(w.shape, BF) for w in weights]
        + [
            DMA((6,)), DMA((count,)), DMA((count,)), DMA((count, ny)), DMA((count, ny)),
            DMA((count, ny)), DMA((count, ny)),
        ],
        compiler_params=params(0),
        name="project",
    )(
        tokens, pre_gain[None], q_norm_gain[None], kv_norm_gain[None], cos_full, sin_full, *weights
    )

    query = lax.dot_general(
        q_up_weight, q_normed, (((0,), (1,)), ((), ())), preferred_element_type=F32
    ).reshape(heads, NOPE + ROPE, rows)
    first, second = query[:, NOPE : NOPE + ROPE // 2], query[:, NOPE + ROPE // 2 :]
    ct, st = cosine.T[None], sine.T[None]
    qt = jnp.concatenate(
        [
            query[:, :NOPE], jnp.zeros((heads, VDIM, rows), F32),
            first * ct - second * st, second * ct + first * st,
            jnp.zeros((heads, LANES - ROPE, rows), F32),
        ],
        axis=1,
    ).astype(BF)

    attended, log_total = pl.pallas_call(
        functools.partial(attend_kernel, nz, nx, ntp, heads),
        out_shape=[struct((rows, heads * VDIM), BF), struct((heads, rows), F32)],
        in_specs=vmem(3),
        out_specs=vmem(2),
        scratch_shapes=[
            pltpu.VMEM((nsp, rows, kv_rank + LANES), BF),
            pltpu.VMEM((heads, rows, LANES), BF),
            pltpu.VMEM((heads, LANES, rows), F32),
            pltpu.VMEM((heads, 1, rows), F32),
            pltpu.VMEM((heads, 1, rows), F32),
            DMA((nz,)), DMA((nz, nx)), DMA((nsp,)), DMA((nsp,)), DMA((nsp,)),
        ],
        compiler_params=params(1),
        name="attend",
    )(kvb, qt, kv_up_weight)

    prior = lax.ppermute(driven[rows - (TAPS - 1) :], "sp", [(i, i + 1) for i in range(nsp - 1)])
    extended = jnp.concatenate([prior, driven], axis=0)
    convolved = jnp.zeros(driven.shape, F32)
    for index in range(TAPS):
        convolved = convolved + conv_taps[index].astype(F32) * extended[
            index : index + rows
        ].astype(F32)
    conv_branch = (outer.astype(F32) * convolved).astype(BF)

    block = (ny, rows, width)
    mixed = pl.pallas_call(
        functools.partial(finish_kernel, ntp, chunk),
        out_shape=struct((rows, width), BF),
        in_specs=vmem(5),
        out_specs=pl.BlockSpec(memory_space=pltpu.VMEM),
        scratch_shapes=[pltpu.VMEM(block, BF)] * 5
        + [
            pltpu.VMEM((rows, width), BF), pltpu.VMEM((rows, width), BF),
            pltpu.VMEM((rows, width), F32),
            pltpu.VMEM((8, rows), F32), pltpu.VMEM((ntp, 8, rows), F32),
            DMA((count, ny)), DMA((count, ny)), DMA((count, ny)), DMA((count, ny)),
            DMA((count,)), DMA((count,)), DMA((ntp,)), DMA((ntp,)),
        ],
        compiler_params=params(2),
        name="finish",
    )(attended, conv_branch, attn_out_weight, conv_out_weight, post_gain[None])
    return mixed, log_total


def solution(mesh):
    placed = (
        P("sp", "tp"), P(), P(None, "tp"), P(None, "tp"), P(None, "tp"), P(None, "tp"), P(), P(),
        P(None, "tp"), P(), P(), P(), P(None, "tp"), P("tp", None), P("tp", None), P("tp"),
    )
    return jax.shard_map(
        functools.partial(body, mesh.shape["sp"], mesh.shape["tp"]),
        mesh=mesh,
        in_specs=placed,
        out_specs=(P("sp", "tp"), P("tp", "sp")),
        check_vma=False,
    )
```

```python
import functools
import math

import jax
import jax.numpy as jnp
from jax import lax
from jax.experimental import pallas as pl
from jax.experimental.pallas import tpu as pltpu
from jax.sharding import PartitionSpec as P

NOPE = 64
ROPE = 32
VDIM = 64
TAPS = 3
LANES = 128

EPSILON = 1e-06
THETA = 500000.0
NEGATIVE = -1e30
MESH = pl.DeviceIdType.MESH
BF = jnp.bfloat16
F32 = jnp.float32


def remote(src, dst, send, recv, **where):
    return pltpu.make_async_remote_copy(
        src_ref=src, dst_ref=dst, send_sem=send, recv_sem=recv, device_id=where, device_id_type=MESH
    )


def dot(a, b):
    return jnp.dot(a, b, preferred_element_type=F32)


def greet_tp(tp, n):
    barrier = pltpu.get_barrier_semaphore()
    for step in range(1, n):
        pl.semaphore_signal(
            barrier, inc=1, device_id={"tp": lax.rem(tp + step, n)}, device_id_type=MESH
        )
    pl.semaphore_wait(barrier, n - 1)


def project_kernel(
    n, chunk,
    tok, pre, qg, kg, cos, sin, wo, wi, ws, wq, wk, wr,
    outer, driven, qn, kvb,
    buf, vo, vi, vs, vq, vk, vr, wsem, own_s, own_r, y_s, y_r, f_s, f_r,
):
    tp = lax.axis_index("tp")
    ny = n // 2
    y, core = tp // 2, lax.rem(tp, 2)
    partner = tp + 1 - 2 * core
    rows, width = tok.shape
    count = rows // chunk
    loads = [
        pltpu.make_async_copy(a, b, wsem.at[i])
        for i, (a, b) in enumerate(((wo, vo), (wi, vi), (ws, vs), (wq, vq), (wk, vk), (wr, vr)))
    ]
    greet_tp(tp, n)

    def part(r):
        return pl.ds(r * chunk, chunk)

    def y_copy(r, step):
        to = lax.rem(y + step, ny) * 2 + core
        return remote(
            tok.at[part(r)], buf.at[tp, part(r)], y_s.at[r, step], y_r.at[r, y], tp=to
        )

    def y_arrival(r, other):
        return remote(
            tok.at[part(r)], buf.at[other * 2 + core, part(r)], y_s.at[r, 0], y_r.at[r, other],
            tp=partner,
        )

    def own_copy(r):
        return remote(tok.at[part(r)], buf.at[tp, part(r)], own_s.at[r], own_r.at[r], tp=partner)

    def forward(r, other):
        here = buf.at[other * 2 + core, part(r)]
        return remote(here, here, f_s.at[r, other], f_r.at[r, other], tp=partner)

    for r in range(count):
        for step in range(1, ny):
            y_copy(r, step).start()
    for r in range(count):
        own_copy(r).start()
    for load in loads:
        load.start()
    buf[tp] = tok[...]
    for load in loads:
        load.wait()

    def compute(r, carry):
        for step in range(1, ny):
            other = lax.rem(y + ny - step, ny)
            y_arrival(r, other).wait_recv()
            forward(r, other).start()
        own_copy(r).wait_recv()
        for step in range(1, ny):
            other = lax.rem(y + ny - step, ny)
            forward(r, other).wait_recv()
        here = pl.ds(pl.multiple_of(r * chunk, chunk), chunk)
        total = n * width
        wide = jnp.concatenate([buf[s, here] for s in range(n)], axis=1).astype(F32)
        factor = lax.rsqrt(jnp.sum(wide * wide, axis=1, keepdims=True) / total + EPSILON)
        scaled = (wide * pre[...]).astype(BF)
        kv = dot(scaled, vk[...]) * factor
        kv = kv * lax.rsqrt(jnp.mean(kv * kv, axis=1, keepdims=True) + EPSILON) * kg[...]
        rank = kv.shape[1]
        kvb[here, :rank] = kv.astype(BF)
        turn = factor * lax.dot_general(
            scaled, vr[...], (((1,), (1,)), ((), ())), preferred_element_type=F32
        )
        swapped = jnp.concatenate([turn[:, ROPE // 2 :], turn[:, : ROPE // 2]], axis=1)
        turn = turn * cos[:, here].T + swapped * sin[:, here].T
        kvb[here, rank:] = jnp.concatenate(
            [turn, jnp.zeros((chunk, LANES - ROPE), F32)], axis=1
        ).astype(BF)
        q = dot(scaled, vq[...]) * factor
        q = q * lax.rsqrt(jnp.mean(q * q, axis=1, keepdims=True) + EPSILON) * qg[...]
        qn[here] = q.astype(BF)
        outer[here] = (dot(scaled, vo[...]) * factor).astype(BF)
        inner = (dot(scaled, vi[...]) * factor).astype(BF).astype(F32)
        source = (dot(scaled, vs[...]) * factor).astype(BF).astype(F32)
        driven[here] = (inner * source).astype(BF)
        return carry

    lax.fori_loop(0, count, compute, 0)
    for r in range(count):
        own_copy(r).wait_send()
        for step in range(1, ny):
            y_copy(r, step).wait_send()
            forward(r, lax.rem(y + step, ny)).wait_send()


def attend_kernel(
    nz, nx, ntp, heads,
    kvb, qt, up,
    att, logs,
    buf, kv, acc, top, low, z_s, x_s, d_s, i_r, d_r,
):
    sp, tp = lax.axis_index("sp"), lax.axis_index("tp")
    z, x = sp // nx, lax.rem(sp, nx)
    core = lax.rem(tp, 2)
    partner = tp + 1 - 2 * core
    rows = kvb.shape[0]
    half = rows // 2
    rank = up.shape[0]
    scale = (NOPE + ROPE) ** (-0.5)
    factor = scale * math.log2(math.e)
    mine = pl.ds(pl.multiple_of(core * half, half), half)

    barrier = pltpu.get_barrier_semaphore()

    def greet(**where):
        pl.semaphore_signal(barrier, inc=1, device_id=where, device_id_type=MESH)

    greet(tp=partner)
    for step in range(1, nx):
        greet(sp=z * nx + lax.rem(x + step, nx))

    @pl.when(z > 0)
    def _():
        greet(sp=sp - nx)

    @pl.when(z < nz - 1)
    def _():
        greet(sp=sp + nx)

    inside = jnp.where(z > 0, 1, 0) + jnp.where(z < nz - 1, 1, 0)
    pl.semaphore_wait(barrier, nx + inside)

    def up_copy(k):
        src = sp - k * nx
        return remote(buf.at[src, mine], buf.at[src, mine], z_s.at[k], i_r.at[src], sp=sp + nx)

    def side_copy(k, step):
        src = sp - k * nx
        to = z * nx + lax.rem(x + step, nx)
        return remote(buf.at[src, mine], buf.at[src, mine], x_s.at[k, step], i_r.at[src], sp=to)

    def own_up():
        return remote(kvb.at[mine], buf.at[sp, mine], z_s.at[0], i_r.at[sp], sp=sp + nx)

    def own_side(step):
        to = z * nx + lax.rem(x + step, nx)
        return remote(kvb.at[mine], buf.at[sp, mine], x_s.at[0, step], i_r.at[sp], sp=to)

    def arrival(src):
        return remote(kvb.at[mine], buf.at[src, mine], z_s.at[0], i_r.at[src], tp=partner)

    def share(src):
        return remote(buf.at[src, mine], buf.at[src, mine], d_s.at[src], d_r.at[src], tp=partner)

    @pl.when(z < nz - 1)
    def _():
        own_up().start()

    for step in range(1, nx):
        @pl.when(x + step < nx)
        def _(step=step):
            own_side(step).start()

    def compute(block, first):
        lat = block[:, :rank]
        turn = block[:, rank:]
        for h in range(0, heads, 2):
            both = dot(lat, up[:, h * LANES : (h + 2) * LANES]).astype(BF)
            kv[h] = both[:, :LANES]
            kv[h + 1] = both[:, LANES:]

        def one(h):
            keyval = kv[h]
            scores = dot(jnp.concatenate([keyval, turn], axis=1), qt[h])
            if first:
                key = lax.broadcasted_iota(jnp.int32, scores.shape, 0)
                query = lax.broadcasted_iota(jnp.int32, scores.shape, 1)
                scores = jnp.where(key <= query, scores, NEGATIVE)
            peak = jnp.max(scores, axis=0, keepdims=True) * factor
            if not first:
                before = top[h]
                peak = jnp.maximum(before, peak)
            weights = jnp.exp2(scores * factor - peak)
            total = jnp.sum(weights, axis=0, keepdims=True)
            values = lax.dot_general(
                keyval, weights.astype(BF), (((0,), (0,)), ((), ())), preferred_element_type=F32
            )
            if not first:
                shrink = jnp.exp2(before - peak)
                total = total + low[h] * shrink
                values = values + acc[h] * shrink
            top[h] = peak
            low[h] = total
            acc[h] = values

        def pair(i, carry):
            one(2 * i)
            one(2 * i + 1)
            return carry

        lax.fori_loop(0, heads // 2, pair, 0)

    compute(kvb[...], True)

    def side_source(k, step):
        return (z - k) * nx + lax.rem(x + step, nx)

    def side_share(k, low_step):
        def run(step, carry):
            src = side_source(k, step)
            arrival(src).wait_recv()
            share(src).start()
            return carry

        lax.fori_loop(low_step, nx, run, 0)

    def shared_compute(src):
        share(src).wait_recv()
        compute(buf[src], False)

    def level(k, carry):
        src = sp - k * nx
        fresh = k <= z

        @pl.when(fresh)
        def _():
            arrival(src).wait_recv()
            share(src).start()

            @pl.when(z < nz - 1)
            def _():
                up_copy(k).start()

            for step in range(1, nx):
                side_copy(k, step).start()

        low_step = jnp.where(k == 1, nx - x, 1)
        side_share(k - 1, low_step)

        def run(step, carry):
            shared_compute(jnp.where(step == 0, src, side_source(k - 1, step + low_step - 1)))
            return carry

        lax.fori_loop(jnp.where(fresh, 0, 1), nx - low_step + 1, run, 0)
        return carry

    lax.fori_loop(1, z + 2, level, 0)

    for i in range(heads // 2):
        both = jnp.concatenate(
            [acc[2 * i, NOPE:] / low[2 * i], acc[2 * i + 1, NOPE:] / low[2 * i + 1]], axis=0
        )
        att[:, i * LANES : (i + 1) * LANES] = both.T.astype(BF)
    for h in range(heads):
        logs[h : h + 1, :] = top[h] * math.log(2.0) + jnp.log(low[h])

    @pl.when(z < nz - 1)
    def _():
        own_up().wait_send()

    for step in range(1, nx):
        @pl.when(x + step < nx)
        def _(step=step):
            own_side(step).wait_send()

    def side_sent(k, low_step):
        def run(step, carry):
            share((z - k) * nx + lax.rem(x + step, nx)).wait_send()
            return carry

        lax.fori_loop(low_step, nx, run, 0)

    side_sent(0, nx - x)

    def sent(k, carry):
        @pl.when(z < nz - 1)
        def _():
            up_copy(k).wait_send()

        for step in range(1, nx):
            side_copy(k, step).wait_send()
        share(sp - k * nx).wait_send()
        side_sent(k, 1)
        return carry

    lax.fori_loop(1, z + 1, sent, 0)


def finish_kernel(
    n, chunk,
    att, conv, wa, wc, gain,
    out,
    away, mine, pin, ysend, yin, peer, pown, total, sq, sqin,
    a_s, a_r, y_s, y_r, p_s, p_r, q_s, q_r,
):
    tp = lax.axis_index("tp")
    ny = n // 2
    y, core = tp // 2, lax.rem(tp, 2)
    partner = tp + 1 - 2 * core
    rows, width = out.shape
    count = rows // chunk
    greet_tp(tp, n)

    def part(r):
        return pl.ds(r * chunk, chunk)

    def product(r, dest):
        columns = pl.ds(pl.multiple_of(dest * width, width), width)
        return (dot(att[part(r)], wa[:, columns]) + dot(conv[part(r)], wc[:, columns])).astype(BF)

    def to_partner(r, step):
        return remote(
            away.at[step, part(r)], pin.at[step, part(r)], a_s.at[r, step], a_r.at[r, step], tp=partner
        )

    def across(r, step):
        to = lax.rem(y + step, ny) * 2 + core
        return remote(
            ysend.at[step, part(r)], yin.at[step, part(r)], y_s.at[r, step], y_r.at[r, step], tp=to
        )

    def home(r):
        return remote(peer.at[part(r)], pown.at[part(r)], p_s.at[r], p_r.at[r], tp=partner)

    def squares(step):
        return remote(
            sq, sqin.at[step], q_s.at[step], q_r.at[step], tp=lax.rem(tp + step, n)
        )

    for r in range(count):
        for step in range(1, ny):
            dest = lax.rem(y + step, ny) * 2
            away[step, part(r)] = product(r, dest + 1 - core)
            to_partner(r, step).start()
            mine[step, part(r)] = product(r, dest + core)
    for r in range(count):
        for step in range(1, ny):
            to_partner(r, step).wait_recv()
            ysend[step, part(r)] = (
                mine[step, part(r)].astype(F32) + pin[step, part(r)].astype(F32)
            ).astype(BF)
            across(r, step).start()
    for r in range(count):
        peer[part(r)] = product(r, partner)
        home(r).start()
        total[part(r)] = product(r, tp).astype(F32)
    for r in range(count):
        home(r).wait_recv()
        total[part(r)] += pown[part(r)].astype(F32)
    for r in range(count):
        for step in range(1, ny):
            across(r, step).wait_recv()
            total[part(r)] += yin[step, part(r)].astype(F32)
        value = total[part(r)]
        sums = jnp.sum(value * value, axis=1, keepdims=True)
        sq[:, part(r)] = jnp.broadcast_to(sums, (chunk, LANES)).T[:8]
    for step in range(1, n):
        squares(step).start()
    whole = sq[...]
    for step in range(1, n):
        squares(step).wait_recv()
        whole = whole + sqin[step]
    scale = lax.rsqrt(whole / (n * width) + EPSILON)
    for r in range(count):
        column = jnp.broadcast_to(
            scale[:1, r * chunk : (r + 1) * chunk], (LANES, chunk)
        ).T[:, :1]
        out[part(r)] = (total[part(r)] * column * gain[...]).astype(BF)
    for r in range(count):
        home(r).wait_send()
        for step in range(1, ny):
            to_partner(r, step).wait_send()
            across(r, step).wait_send()
    for step in range(1, n):
        squares(step).wait_send()


def vmem(count):
    return [pl.BlockSpec(memory_space=pltpu.VMEM)] * count


def params(collective):
    return pltpu.CompilerParams(
        collective_id=collective, has_side_effects=True, vmem_limit_bytes=56 * 1024 * 1024
    )


DMA = pltpu.SemaphoreType.DMA


def body(
    nsp, ntp,
    tokens, pre_gain, outer_gate_weight, inner_gate_weight, source_weight, conv_taps,
    q_down_weight, q_norm_gain, q_up_weight, kv_down_weight, rope_key_weight, kv_norm_gain,
    kv_up_weight, attn_out_weight, conv_out_weight, post_gain,
):
    rows, width = tokens.shape
    ny = ntp // 2
    nx = ny if nsp % ny == 0 else 1
    nz = nsp // nx
    chunk = LANES
    count = rows // chunk
    q_rank, kv_rank = q_down_weight.shape[1], kv_down_weight.shape[1]
    channels = outer_gate_weight.shape[1]
    heads = q_up_weight.shape[1] // (NOPE + ROPE)
    struct = jax.ShapeDtypeStruct
    sp = lax.axis_index("sp")

    pos = (sp * rows + jnp.arange(rows, dtype=jnp.int32)).astype(F32)
    freqs = THETA ** (-jnp.arange(0, ROPE, 2, dtype=F32) / ROPE)
    angles = freqs[:, None] * pos[None, :]
    cosine, sine = jnp.cos(angles), jnp.sin(angles)
    cos_full = jnp.concatenate([cosine, cosine], axis=0)
    sin_full = jnp.concatenate([-sine, sine], axis=0)

    weights = (
        outer_gate_weight, inner_gate_weight, source_weight,
        q_down_weight, kv_down_weight, rope_key_weight.T,
    )
    outer, driven, q_normed, kvb = pl.pallas_call(
        functools.partial(project_kernel, ntp, chunk),
        out_shape=[
            struct((rows, channels), BF), struct((rows, channels), BF),
            struct((rows, q_rank), BF), struct((rows, kv_rank + LANES), BF),
        ],
        in_specs=vmem(6) + [pl.BlockSpec(memory_space=pl.ANY)] * 6,
        out_specs=vmem(4),
        scratch_shapes=[pltpu.VMEM((ntp, rows, width), BF)]
        + [pltpu.VMEM(w.shape, BF) for w in weights]
        + [
            DMA((6,)), DMA((count,)), DMA((count,)), DMA((count, ny)), DMA((count, ny)),
            DMA((count, ny)), DMA((count, ny)),
        ],
        compiler_params=params(0),
        name="project",
    )(
        tokens, pre_gain[None], q_norm_gain[None], kv_norm_gain[None], cos_full, sin_full, *weights
    )

    query = lax.dot_general(
        q_up_weight, q_normed, (((0,), (1,)), ((), ())), preferred_element_type=F32
    ).reshape(heads, NOPE + ROPE, rows)
    first, second = query[:, NOPE : NOPE + ROPE // 2], query[:, NOPE + ROPE // 2 :]
    ct, st = cosine[None], sine[None]
    qt = jnp.concatenate(
        [
            query[:, :NOPE], jnp.zeros((heads, VDIM, rows), F32),
            first * ct - second * st, second * ct + first * st,
            jnp.zeros((heads, LANES - ROPE, rows), F32),
        ],
        axis=1,
    ).astype(BF)

    attended, log_total = pl.pallas_call(
        functools.partial(attend_kernel, nz, nx, ntp, heads),
        out_shape=[struct((rows, heads * VDIM), BF), struct((heads, rows), F32)],
        in_specs=vmem(3),
        out_specs=vmem(2),
        scratch_shapes=[
            pltpu.VMEM((nsp, rows, kv_rank + LANES), BF),
            pltpu.VMEM((heads, rows, LANES), BF),
            pltpu.VMEM((heads, LANES, rows), F32),
            pltpu.VMEM((heads, 1, rows), F32),
            pltpu.VMEM((heads, 1, rows), F32),
            DMA((nz,)), DMA((nz, nx)), DMA((nsp,)), DMA((nsp,)), DMA((nsp,)),
        ],
        compiler_params=params(1),
        name="attend",
    )(kvb, qt, kv_up_weight)

    prior = lax.ppermute(driven[rows - (TAPS - 1) :], "sp", [(i, i + 1) for i in range(nsp - 1)])
    extended = jnp.concatenate([prior, driven], axis=0)
    convolved = jnp.zeros(driven.shape, F32)
    for index in range(TAPS):
        convolved = convolved + conv_taps[index].astype(F32) * extended[
            index : index + rows
        ].astype(F32)
    conv_branch = (outer.astype(F32) * convolved).astype(BF)

    block = (ny, rows, width)
    mixed = pl.pallas_call(
        functools.partial(finish_kernel, ntp, chunk),
        out_shape=struct((rows, width), BF),
        in_specs=vmem(5),
        out_specs=pl.BlockSpec(memory_space=pltpu.VMEM),
        scratch_shapes=[pltpu.VMEM(block, BF)] * 5
        + [
            pltpu.VMEM((rows, width), BF), pltpu.VMEM((rows, width), BF),
            pltpu.VMEM((rows, width), F32),
            pltpu.VMEM((8, rows), F32), pltpu.VMEM((ntp, 8, rows), F32),
            DMA((count, ny)), DMA((count, ny)), DMA((count, ny)), DMA((count, ny)),
            DMA((count,)), DMA((count,)), DMA((ntp,)), DMA((ntp,)),
        ],
        compiler_params=params(2),
        name="finish",
    )(attended, conv_branch, attn_out_weight, conv_out_weight, post_gain[None])
    return mixed, log_total


def solution(mesh):
    placed = (
        P("sp", "tp"), P(), P(None, "tp"), P(None, "tp"), P(None, "tp"), P(None, "tp"), P(), P(),
        P(None, "tp"), P(), P(), P(), P(None, "tp"), P("tp", None), P("tp", None), P("tp"),
    )
    return jax.shard_map(
        functools.partial(body, mesh.shape["sp"], mesh.shape["tp"]),
        mesh=mesh,
        in_specs=placed,
        out_specs=(P("sp", "tp"), P("tp", "sp")),
        check_vma=False,
    )
```
